512 devices in a mesh: sp: 32 (over z, x), tp: 16 (over y, core).
Axes of the slice: x: 4, y: 8, z: 8, core: 2. Of those that a mesh axis runs over, the one named last changes fastest.
Arguments:
- latent: bfloat16 [16384, 2048], P('sp'), may hold values from -6 to 6
- context: bfloat16 [512, 2048], P('sp'), may hold values from -6 to 6
- condition: bfloat16 [2048], replicated, may hold values from -6 to 6
- context_condition: bfloat16 [2048], replicated, may hold values from -6 to 6
- shift_weight: bfloat16 [2048, 2048], P('sp', 'tp'), may hold values from -0.125 to 0.125
- scale_weight: bfloat16 [2048, 2048], P('sp', 'tp'), may hold values from -0.125 to 0.125
- mod_gate_weight: bfloat16 [2048, 2048], P('sp', 'tp'), may hold values from -0.5 to 0.5
- norm_gain: bfloat16 [2048], replicated, may hold values from 0.099609375 to 1.8984375
- query_weight: bfloat16 [2048, 2048], P(None, 'tp'), may hold values from -0.125 to 0.125
- key_weight: bfloat16 [2048, 2048], P(None, 'tp'), may hold values from -0.125 to 0.125
- value_weight: bfloat16 [2048, 2048], P(None, 'tp'), may hold values from -0.125 to 0.125
- gate_weight: bfloat16 [2048, 2048], P(None, 'tp'), may hold values from -0.125 to 0.125
- forward_decay: float32 [16], P('tp'), may hold values from 0 to 1, as said below
- backward_decay: float32 [16], P('tp'), may hold values from 0 to 1, as said below
- out_weight: bfloat16 [2048, 2048], P('tp'), may hold values from -0.125 to 0.125
Outputs:
- mixed: bfloat16 [16384, 2048], P('sp')
The draws below stay inside these ranges and needn't reach their ends.
Inputs may be any that keep to these rules, and one draw needn't show every extreme that they name: `forward_decay`: each head's rate is positive. `backward_decay`: each head's rate is positive.
All inputs are finite; a program needn't handle non-finite values.
Results may differ from the reference program's by a relative error of at most 0.015.
Values may be sent and summed in bfloat16 or wider, within the bound.
No kernel may reach another device: no remote copies, remote signals or barrier semaphores. Data moves between devices by JAX's collectives and lax.ppermute only.
A program may use at most 64 MiB of HBM per device.

```python
import jax
import jax.numpy as jnp
from jax import lax

D = 2048
HEAD_DIM = 128
RET_HEADS = 16
RET_WIDTH = 2048
GRID_W = 64
SEQ = 16384
CTX = 512


def decay_rates(key, fast_share):
    pick_key, fast_key, slow_key = jax.random.split(key, 3)
    fast = jax.random.uniform(pick_key, (RET_HEADS,), jnp.float32) < fast_share
    fast_rate = jnp.exp(jax.random.uniform(fast_key, (RET_HEADS,), jnp.float32, jnp.log(1.0 / 100.0), jnp.log(1.0 / 30.0)))
    slow_rate = jnp.exp(jax.random.uniform(slow_key, (RET_HEADS,), jnp.float32, jnp.log(0.2), jnp.log(2.0))) / SEQ
    return jnp.where(fast, fast_rate, slow_rate).astype(jnp.float32)


def draw_forward_decay(key, part):
    share = 0.5
    return decay_rates(jax.random.fold_in(key, 11), share)


def draw_backward_decay(key, part):
    share = 0.5
    return decay_rates(jax.random.fold_in(key, 23), share)


def level_of(key, extent, cuts, smallest, top_value):
    loudness = 1.0
    for position, blocks in cuts:
        heights = jax.random.uniform(jax.random.fold_in(jax.random.fold_in(key, 6), position), (blocks,), jnp.float32, smallest / len(cuts), top_value / len(cuts))
        loudness = loudness * jnp.repeat(jnp.exp(heights), extent[position] // blocks).reshape((-1,) + (1,) * (len(extent) - 1 - position))
    return loudness


def noise(key, shape, scale, bound, cuts=(), kind=jnp.bfloat16):
    drawn = jax.random.normal(key, shape, jnp.float32) * scale
    if len(cuts) > 0:
        drawn = level_of(key, shape, cuts, -0.22, 0.18) * drawn
    return jnp.clip(drawn, min=-bound, max=bound).astype(kind)


def setup_inputs(seed: int = 0) -> dict:
    streams_of = jax.random.split(jax.random.key(seed), 16)
    latent = noise(streams_of[0], (SEQ, D), 1.0, 6.0, ((0, 32),))
    context = noise(streams_of[1], (CTX, D), 1.0, 6.0, ((0, 32),))
    condition = noise(streams_of[2], (D,), 1.0, 6.0)
    context_condition = noise(streams_of[3], (D,), 1.0, 6.0)
    shift_weight = noise(streams_of[4], (D, D), D ** -0.5, 0.125, ((0, 32), (1, 16)))
    scale_weight = noise(streams_of[5], (D, D), D ** -0.5, 0.125, ((0, 32), (1, 16)))
    mod_gate_weight = noise(streams_of[6], (D, D), (D // 16) ** -0.5, 0.5, ((0, 32), (1, 16)))
    norm_gain = jnp.clip(1.0 + 0.18 * jax.random.normal(streams_of[7], (D,), jnp.float32), 0.099609375, 1.8984375).astype(jnp.bfloat16)
    query_weight = noise(streams_of[8], (D, RET_WIDTH), D ** -0.5, 0.125, ((1, 16),))
    key_weight = noise(streams_of[9], (D, RET_WIDTH), D ** -0.5, 0.125, ((1, 16),))
    value_weight = noise(streams_of[10], (D, RET_WIDTH), D ** -0.5, 0.125, ((1, 16),))
    gate_weight = noise(streams_of[11], (D, RET_WIDTH), D ** -0.5, 0.125, ((1, 16),))
    forward_decay = draw_forward_decay(jax.random.fold_in(streams_of[15], 71), 0)
    backward_decay = draw_backward_decay(jax.random.fold_in(streams_of[15], 71), 0)
    out_weight = noise(streams_of[14], (RET_WIDTH, D), RET_WIDTH ** -0.5, 0.125, ((0, 16),))
    return dict(latent=latent, context=context, condition=condition, context_condition=context_condition, shift_weight=shift_weight, scale_weight=scale_weight, mod_gate_weight=mod_gate_weight, norm_gain=norm_gain, query_weight=query_weight, key_weight=key_weight, value_weight=value_weight, gate_weight=gate_weight, forward_decay=forward_decay, backward_decay=backward_decay, out_weight=out_weight)


EPS = 1e-06
THETA = 10000.0
CONTEXT_LIFT = 3.0
TOP_PRECISION = lax.Precision.HIGHEST

def modulated(token_rows, norm_gain, shifts, scales):
    values = token_rows.astype(jnp.float32)
    values = values * lax.rsqrt(lax.optimization_barrier(jnp.mean(values * values, axis=-1, keepdims=True)) + EPS)
    values = values * norm_gain.astype(jnp.float32)
    return (values * (1.0 + scales) + shifts).astype(jnp.bfloat16)

def rope_half(portion, positions):
    quarter = portion.shape[-1] // 2
    frequency = THETA ** (-jnp.arange(quarter, dtype=jnp.float32) / quarter)
    angles = positions[:, None, None] * frequency
    cosine = jnp.cos(angles)
    sine_table = jnp.sin(angles)
    leading = portion[..., :quarter]
    trailing = portion[..., quarter:]
    return jnp.concatenate([leading * cosine - trailing * sine_table, leading * sine_table + trailing * cosine], axis=-1)

def rotate(values, grid_row, grid_column):
    half_width = values.shape[-1] // 2
    return jnp.concatenate([rope_half(values[..., :half_width], grid_row), rope_half(values[..., half_width:], grid_column)], axis=-1)

def blockwise(query_heads, key_heads, value_heads, log_decay, initial):
    head_count, length, head_width = query_heads.shape
    block_rows = 128
    block_count = length // block_rows

    def to_blocks(values):
        return jnp.moveaxis(values.reshape(head_count, block_count, block_rows, head_width), 1, 0)
    offsets = jnp.arange(block_rows, dtype=jnp.float32)
    distance = offsets[:, None] - offsets[None, :]
    within_block_decay = jnp.where(distance >= 0, jnp.exp(log_decay[:, None, None] * jnp.maximum(distance, 0.0)), 0.0)
    query_decay = jnp.exp(log_decay[:, None] * (offsets + 1.0))[:, :, None]
    key_decay_factor = jnp.exp(log_decay[:, None] * (block_rows - 1.0 - offsets))[:, :, None]
    per_step_decay = jnp.exp(log_decay * block_rows)[:, None, None]

    def advance(carried_state, pieces):
        query_tile_rows, key_tile_rows, value_tile_rows = pieces
        score_matrix = jnp.einsum('fya,fqa->fyq', query_tile_rows, key_tile_rows, precision=TOP_PRECISION) * within_block_decay
        result_output = jnp.einsum('rij,rjy->riy', score_matrix, value_tile_rows, precision=TOP_PRECISION)
        result_output = result_output + jnp.einsum('hnd,hde->hne', query_tile_rows, carried_state, precision=TOP_PRECISION) * query_decay
        carried_state = carried_state * per_step_decay + jnp.einsum('cwz,cwu->czu', key_tile_rows * key_decay_factor, value_tile_rows, precision=TOP_PRECISION)
        return (carried_state, result_output)
    _, outputs = lax.scan(advance, initial, (to_blocks(query_heads), to_blocks(key_heads), to_blocks(value_heads)))
    return jnp.moveaxis(outputs, 0, 1).reshape(head_count, length, head_width)

def reference(latent, context, condition, context_condition, shift_weight, scale_weight, mod_gate_weight, norm_gain, query_weight, key_weight, value_weight, gate_weight, forward_decay, backward_decay, out_weight):
    activation = jax.nn.silu(jnp.stack([condition, context_condition]).astype(jnp.float32)).astype(jnp.bfloat16)
    shifts = jnp.dot(activation, shift_weight, preferred_element_type=jnp.float32)
    scales = jnp.dot(activation, scale_weight, preferred_element_type=jnp.float32)
    gates = jnp.dot(activation, mod_gate_weight, preferred_element_type=jnp.float32)
    hidden = modulated(latent, norm_gain, shifts[0], scales[0])
    context_hidden = modulated(context, norm_gain, shifts[1], scales[1])
    queries = jnp.dot(hidden, query_weight, preferred_element_type=jnp.float32).astype(jnp.bfloat16)
    keys_out = jnp.dot(hidden, key_weight, preferred_element_type=jnp.float32).astype(jnp.bfloat16)
    values_out = jnp.dot(hidden, value_weight, preferred_element_type=jnp.float32).astype(jnp.bfloat16)
    out_gates = jnp.dot(hidden, gate_weight, preferred_element_type=jnp.float32).astype(jnp.bfloat16)
    context_keys = jnp.dot(context_hidden, key_weight, preferred_element_type=jnp.float32).astype(jnp.bfloat16)
    context_values = jnp.dot(context_hidden, value_weight, preferred_element_type=jnp.float32).astype(jnp.bfloat16)
    length = latent.shape[0]
    positions = jnp.arange(length, dtype=jnp.int32)
    grid_row = (positions // GRID_W).astype(jnp.float32)
    grid_column = (positions % GRID_W).astype(jnp.float32)
    key_scale = HEAD_DIM ** (-0.5)

    def to_heads(values):
        return values.astype(jnp.float32).reshape(values.shape[0], RET_HEADS, HEAD_DIM)
    query_heads = jnp.transpose(rotate(to_heads(queries), grid_row, grid_column), (1, 0, 2))
    key_heads = jnp.transpose(rotate(to_heads(keys_out), grid_row, grid_column), (1, 0, 2)) * key_scale
    value_heads = jnp.transpose(to_heads(values_out), (1, 0, 2))
    log_forward = -forward_decay.astype(jnp.float32)
    log_backward = -backward_decay.astype(jnp.float32)
    context_index = jnp.arange(CTX, dtype=jnp.float32)
    weight_forward = jnp.exp(log_forward[:, None] * (CTX - 1.0 - context_index)[None, :])
    weight_backward = jnp.exp(log_backward[:, None] * context_index[None, :])
    context_key_heads = to_heads(context_keys) * (key_scale * CONTEXT_LIFT)
    context_value_heads = to_heads(context_values)
    context_forward = jnp.einsum('hc,chd,che->hde', weight_forward, context_key_heads, context_value_heads, precision=TOP_PRECISION)
    context_backward = jnp.einsum('hc,chd,che->hde', weight_backward, context_key_heads, context_value_heads, precision=TOP_PRECISION)
    forward_out = blockwise(query_heads, key_heads, value_heads, log_forward, context_forward)
    backward_out = blockwise(jnp.flip(query_heads, 1), jnp.flip(key_heads, 1), jnp.flip(value_heads, 1), log_backward, context_backward)
    retained = forward_out + jnp.flip(backward_out, 1)
    retained = retained * lax.rsqrt(lax.optimization_barrier(jnp.mean(retained * retained, axis=-1, keepdims=True)) + EPS)
    merged = jnp.transpose(retained, (1, 0, 2)).reshape(length, RET_HEADS * HEAD_DIM)
    heads_out = (jax.nn.silu(out_gates.astype(jnp.float32)) * merged).astype(jnp.bfloat16)
    projection = jnp.dot(heads_out, out_weight, preferred_element_type=jnp.float32)
    return (latent.astype(jnp.float32) + gates[0] * projection).astype(jnp.bfloat16)
```

```python
import jax
import jax.numpy as jnp
from jax import lax
from jax.experimental import pallas as pl
from jax.experimental.pallas import tpu as pltpu
from jax.sharding import Mesh
from jax.sharding import PartitionSpec as P

HEAD_DIM = 128
GRID_W = 64
SP = ("z", "x")
TP = ("y", "c")
EPS = 1e-06
THETA = 10000.0
CONTEXT_LIFT = 3.0
BF = jnp.bfloat16
F32 = jnp.float32


def dot(a, b, dims):
    return lax.dot_general(a, b, (dims, ((), ())), preferred_element_type=F32)


def spread(x, axes):
    copies = jnp.broadcast_to(x, (lax.axis_size(axes), *x.shape))
    return lax.all_to_all(copies, axes, split_axis=0, concat_axis=0, tiled=True)


def modulated(rows, gain, shift, scale):
    v = rows.astype(F32)
    v = v * lax.rsqrt(jnp.mean(v * v, axis=-1, keepdims=True) + EPS)
    return (v * gain * (1.0 + scale) + shift).astype(BF)


def rope_tables(start, count):
    quarter = HEAD_DIM // 4
    freq = THETA ** (-jnp.arange(quarter, dtype=F32) / quarter)
    rows = count // GRID_W
    row_angle = (start // GRID_W + jnp.arange(rows, dtype=jnp.int32)).astype(F32)[:, None] * freq
    col_angle = jnp.arange(GRID_W, dtype=jnp.int32).astype(F32)[:, None] * freq

    def table(fn, sign):
        r = fn(row_angle)
        c = fn(col_angle)
        r2 = jnp.broadcast_to(
            jnp.concatenate([sign * r, r], 1)[:, None], (rows, GRID_W, 2 * quarter)
        )
        c2 = jnp.broadcast_to(
            jnp.concatenate([sign * c, c], 1)[None], (rows, GRID_W, 2 * quarter)
        )
        return jnp.concatenate([r2, c2], -1).reshape(count, HEAD_DIM)

    return table(jnp.cos, 1.0), table(jnp.sin, -1.0)


def swapped(v):
    q = HEAD_DIM // 4
    return jnp.concatenate(
        [v[:, q : 2 * q], v[:, :q], v[:, 3 * q :], v[:, 2 * q : 3 * q]], axis=1
    )


def project_body(h_ref, w_ref, latent_ref, gate_ref, out_ref):
    acc = dot(h_ref[0], w_ref[0], ((1,), (0,)))
    for k in range(1, h_ref.shape[0]):
        acc = acc + dot(h_ref[k], w_ref[k], ((1,), (0,)))
    out_ref[...] = (latent_ref[...].astype(F32) + gate_ref[...] * acc).astype(BF)


def project(heads, weight, latent, gate):
    groups, rows, width = heads.shape
    cols = weight.shape[2]
    tile = min(512, cols)
    return pl.pallas_call(
        project_body,
        grid=(cols // tile,),
        in_specs=[
            pl.BlockSpec((groups, rows, width), lambda j: (0, 0, 0)),
            pl.BlockSpec((groups, width, tile), lambda j: (0, 0, j)),
            pl.BlockSpec((rows, tile), lambda j: (0, j)),
            pl.BlockSpec((1, tile), lambda j: (0, j)),
        ],
        out_specs=pl.BlockSpec((rows, tile), lambda j: (0, j)),
        out_shape=jax.ShapeDtypeStruct((rows, cols), BF),
        name="project",
    )(heads, weight, latent, gate)


def local(
    latent,
    context,
    condition,
    context_condition,
    shift_weight,
    scale_weight,
    mod_gate_weight,
    norm_gain,
    query_weight,
    key_weight,
    value_weight,
    gate_weight,
    forward_decay,
    backward_decay,
    out_weight,
):
    z, x = lax.axis_index("z"), lax.axis_index("x")
    nz, nx = lax.axis_size("z"), lax.axis_size("x")
    sp_index, sp_count = lax.axis_index(SP), nz * nx
    tokens = latent.shape[0]
    context_rows = context.shape[0]
    mod_rows = shift_weight.shape[0]

    full_weight = lax.all_gather(out_weight, TP, axis=0, tiled=False)

    activation = jax.nn.silu(jnp.stack([condition, context_condition]).astype(F32)).astype(BF)
    own = lax.dynamic_slice_in_dim(activation, sp_index * mod_rows, mod_rows, 1)
    partial = jnp.concatenate(
        [dot(own, m, ((1,), (0,))) for m in (shift_weight, scale_weight, mod_gate_weight)]
        + [jnp.zeros((2, shift_weight.shape[1]), F32)],
        axis=0,
    )
    summed = jnp.sum(spread(partial, SP), axis=0)
    modulation = spread(summed, TP)
    modulation = jnp.moveaxis(modulation, 0, 1).reshape(8, -1)
    gain = norm_gain.astype(F32)
    hidden = modulated(latent, gain, modulation[0], modulation[2])
    context_hidden = modulated(context, gain, modulation[1], modulation[3])

    stacked = jnp.concatenate([query_weight, key_weight, value_weight, gate_weight], axis=1)
    projected = dot(hidden, stacked, ((1,), (0,))).astype(BF)
    pairs = dot(context_hidden, stacked[:, HEAD_DIM : 3 * HEAD_DIM], ((1,), (0,))).astype(BF)
    context_pack = jnp.concatenate([pairs[:, :HEAD_DIM], pairs[:, HEAD_DIM:]], axis=0)

    cosine, sine = rope_tables(sp_index * tokens, tokens)
    scale = HEAD_DIM ** (-0.5)
    q0 = projected[:, :HEAD_DIM].astype(F32)
    k0 = projected[:, HEAD_DIM : 2 * HEAD_DIM].astype(F32)
    v = projected[:, 2 * HEAD_DIM : 3 * HEAD_DIM]
    out_gates = projected[:, 3 * HEAD_DIM :].astype(F32)
    q = q0 * cosine + swapped(q0) * sine
    k = (k0 * cosine + swapped(k0) * sine) * scale
    rate_f, rate_b = forward_decay[0], backward_decay[0]
    at = jnp.arange(tokens, dtype=F32)[:, None]
    state_f = dot((k * jnp.exp(-rate_f * (tokens - 1.0 - at))).astype(BF), v, ((0,), (0,)))
    state_b = dot((k * jnp.exp(-rate_b * at)).astype(BF), v, ((0,), (0,)))
    pack = jnp.concatenate([state_f.astype(BF), state_b.astype(BF), context_pack], axis=0)
    from_x = spread(pack, "x")

    span = float(tokens)
    xs = jnp.arange(nx, dtype=F32)
    xf = x.astype(F32)
    zf = z.astype(F32)
    sf = from_x[:, :HEAD_DIM].astype(F32)
    sb = from_x[:, HEAD_DIM : 2 * HEAD_DIM].astype(F32)
    context_group = from_x[:, 2 * HEAD_DIM :].reshape(-1, HEAD_DIM)

    def weighted(w, s):
        return jnp.sum(w[:, None, None] * s, axis=0)

    def power(rate, steps):
        return jnp.where(steps >= 0, jnp.exp(-rate * span * jnp.maximum(steps, 0.0)), 0.0)

    total_f = weighted(power(rate_f, nx - 1.0 - xs), sf).astype(BF)
    total_b = weighted(power(rate_b, xs), sb).astype(BF)
    before_x = weighted(power(rate_f, xf - 1.0 - xs), sf)
    after_x = weighted(power(rate_b, xs - xf - 1.0), sb)
    zs = jnp.arange(nz, dtype=jnp.int32)
    chosen = jnp.where((zs > z)[:, None, None], total_f[None], total_b[None])
    message = jnp.concatenate(
        [chosen, jnp.broadcast_to(context_group[None], (nz, *context_group.shape))], axis=1
    )
    from_z = lax.all_to_all(message, "z", split_axis=0, concat_axis=0, tiled=True)

    gap = at - jnp.arange(tokens, dtype=F32)[None, :]
    mixing = jnp.exp(jnp.where(gap >= 0, -rate_f * gap, rate_b * gap)) + jnp.where(
        gap == 0, 1.0, 0.0
    )
    scores = (dot(q.astype(BF), k.astype(BF), ((1,), (1,))) * mixing).astype(BF)
    local_out = dot(scores, v, ((1,), (0,)))

    zsf = zs.astype(F32)
    sz = from_z[:, :HEAD_DIM].astype(F32)
    cz = from_z[:, HEAD_DIM:].reshape(sp_count, 2, context_rows, HEAD_DIM)
    ck = cz[:, 0].reshape(-1, HEAD_DIM).astype(F32) * (scale * CONTEXT_LIFT)
    cv = cz[:, 1].reshape(-1, HEAD_DIM)
    total = context_rows * sp_count
    cat = jnp.arange(total, dtype=F32)[:, None]
    context_f = dot((ck * jnp.exp(-rate_f * (total - 1.0 - cat))).astype(BF), cv, ((0,), (0,)))
    context_b = dot((ck * jnp.exp(-rate_b * cat)).astype(BF), cv, ((0,), (0,)))
    block = sp_index.astype(F32)
    incoming_f = (
        before_x
        + weighted(power(rate_f, xf) * power(rate_f, nx * (zf - 1.0 - zsf)), sz)
        + power(rate_f, block) * context_f
    )
    incoming_b = (
        after_x
        + weighted(power(rate_b, nx - 1.0 - xf) * power(rate_b, nx * (zsf - zf - 1.0)), sz)
        + power(rate_b, sp_count - 1.0 - block) * context_b
    )
    read_f = dot(
        (q * jnp.exp(-rate_f * (at + 1.0))).astype(BF), incoming_f.astype(BF), ((1,), (0,))
    )
    read_b = dot(
        (q * jnp.exp(-rate_b * (tokens - at))).astype(BF), incoming_b.astype(BF), ((1,), (0,))
    )
    retained = local_out + read_f + read_b
    retained = retained * lax.rsqrt(jnp.mean(retained * retained, axis=-1, keepdims=True) + EPS)
    heads = (jax.nn.silu(out_gates) * retained).astype(BF)
    all_heads = lax.all_gather(heads, TP, axis=0, tiled=False)
    return project(all_heads, full_weight, latent, modulation[4:5])


def solution(mesh):
    torus = Mesh(mesh.devices.reshape(8, 4, 8, 2), ("z", "x", "y", "c"))
    rows, cols = P(SP, None), P(None, TP)
    both = P(SP, TP)
    in_specs = (
        (rows, rows, P(), P(), both, both, both, P(), cols, cols, cols, cols)
        + (P(TP), P(TP), P(TP, None))
    )
    return jax.shard_map(local, mesh=torus, in_specs=in_specs, out_specs=rows, check_vma=False)
```

```python
import jax
import jax.numpy as jnp
from jax import lax
from jax.experimental import pallas as pl
from jax.experimental.pallas import tpu as pltpu
from jax.sharding import Mesh
from jax.sharding import PartitionSpec as P

HEAD_DIM = 128
GRID_W = 64
SP = ("z", "x")
TP = ("y", "c")
EPS = 1e-06
THETA = 10000.0
CONTEXT_LIFT = 3.0
BF = jnp.bfloat16
F32 = jnp.float32


def dot(a, b, dims):
    return lax.dot_general(a, b, (dims, ((), ())), preferred_element_type=F32)


def rope_tables(start, count):
    quarter = HEAD_DIM // 4
    freq = THETA ** (-jnp.arange(quarter, dtype=F32) / quarter)
    rows = count // GRID_W
    row_angle = (start // GRID_W + jnp.arange(rows, dtype=jnp.int32)).astype(F32)[:, None] * freq
    col_angle = jnp.arange(GRID_W, dtype=jnp.int32).astype(F32)[:, None] * freq

    def table(fn, sign):
        r = fn(row_angle)
        c = fn(col_angle)
        r2 = jnp.broadcast_to(
            jnp.concatenate([sign * r, r], 1)[:, None], (rows, GRID_W, 2 * quarter)
        )
        c2 = jnp.broadcast_to(
            jnp.concatenate([sign * c, c], 1)[None], (rows, GRID_W, 2 * quarter)
        )
        return jnp.concatenate([r2, c2], -1).reshape(count, HEAD_DIM)

    return table(jnp.cos, 1.0), table(jnp.sin, -1.0)


def roll_pairs(v):
    q = HEAD_DIM // 4
    lane = lax.broadcasted_iota(jnp.int32, v.shape, 1)
    low = (lane % (2 * q)) < q
    return jnp.where(low, pltpu.roll(v, HEAD_DIM - q, 1), pltpu.roll(v, q, 1))


def side_by_side(ref, row):
    return jnp.concatenate([ref[k, row : row + 1, :] for k in range(ref.shape[0])], axis=1)


def partial_body(act_ref, at_ref, shift_ref, scale_ref, gate_ref, out_ref):
    own = act_ref[pl.ds(at_ref[0], 1)][0].astype(F32)
    own = (own * (1.0 / (1.0 + jnp.exp(-own)))).astype(BF)
    parts = [dot(own, m[...], ((1,), (0,))) for m in (shift_ref, scale_ref, gate_ref)]
    both = jnp.concatenate(parts + [jnp.zeros_like(parts[0])], axis=0)
    out_ref[...] = jnp.broadcast_to(both[None], out_ref.shape)


def sum_body(in_ref, out_ref):
    total = in_ref[0]
    for k in range(1, in_ref.shape[0]):
        total = total + in_ref[k]
    out_ref[...] = jnp.broadcast_to(total[None], out_ref.shape)


def normed(rows, factor, shift):
    v = rows.astype(F32)
    r = lax.rsqrt(jnp.mean(v * v, axis=-1, keepdims=True) + EPS)
    return (v * r * factor + shift).astype(BF)


def front_body(
    latent_ref,
    context_ref,
    mod_ref,
    gain_ref,
    weight_ref,
    cos_ref,
    sin_ref,
    par_ref,
    message_ref,
    q_ref,
    g_ref,
    local_ref,
    state_ref,
    modgate_ref,
    k_scr,
    v_scr,
):
    step, steps = pl.program_id(0), pl.num_programs(0)
    tile = latent_ref.shape[0]
    tokens = k_scr.shape[0]
    scale = HEAD_DIM ** (-0.5)
    gain = gain_ref[...].astype(F32)
    h = normed(
        latent_ref[...], gain * (1.0 + side_by_side(mod_ref, 2)), side_by_side(mod_ref, 0)
    )
    proj = dot(h, weight_ref[...], ((1,), (0,))).astype(BF)
    at = pl.ds(pl.multiple_of(step * tile, tile), tile)
    cosine, sine = cos_ref[at, :], sin_ref[at, :]
    q0 = proj[:, :HEAD_DIM].astype(F32)
    k0 = proj[:, HEAD_DIM : 2 * HEAD_DIM].astype(F32)
    q_ref[at, :] = q0 * cosine + roll_pairs(q0) * sine
    k_scr[at, :] = (k0 * cosine + roll_pairs(k0) * sine) * scale
    v_scr[at, :] = proj[:, 2 * HEAD_DIM : 3 * HEAD_DIM]
    g_ref[at, :] = proj[:, 3 * HEAD_DIM :]

    @pl.when(step == steps - 1)
    def _():
        rate_f, rate_b, zf = par_ref[0:1, :], par_ref[1:2, :], par_ref[2:3, :]
        hc = normed(
            context_ref[...], gain * (1.0 + side_by_side(mod_ref, 3)), side_by_side(mod_ref, 1)
        )
        pairs = dot(hc, weight_ref[:, HEAD_DIM : 3 * HEAD_DIM], ((1,), (0,))).astype(BF)
        modgate_ref[...] = side_by_side(mod_ref, 4)
        k = k_scr[...]
        v = v_scr[...]
        row = lax.broadcasted_iota(jnp.int32, (tokens, HEAD_DIM), 0).astype(F32)
        state_f = dot((k * jnp.exp(-rate_f * (tokens - 1.0 - row))).astype(BF), v, ((0,), (0,)))
        state_b = dot((k * jnp.exp(-rate_b * row)).astype(BF), v, ((0,), (0,)))
        state_ref[0] = state_f
        state_ref[1] = state_b
        rows = context_ref.shape[0]
        for n in range(message_ref.shape[0]):
            message_ref[n, :HEAD_DIM, :] = jnp.where(zf < n, state_f, state_b).astype(BF)
            message_ref[n, HEAD_DIM : HEAD_DIM + rows, :] = pairs[:, :HEAD_DIM]
            message_ref[n, HEAD_DIM + rows :, :] = pairs[:, HEAD_DIM:]
        kb = k.astype(BF)
        f1, b1 = rate_f[:, :1], rate_b[:, :1]
        for n in range(tokens // tile):
            qb = q_ref[n * tile : (n + 1) * tile, :].astype(BF)
            gap = (
                lax.broadcasted_iota(jnp.int32, (tile, tokens), 0)
                + n * tile
                - lax.broadcasted_iota(jnp.int32, (tile, tokens), 1)
            ).astype(F32)
            mixing = jnp.exp(jnp.where(gap >= 0, -f1 * gap, b1 * gap)) * jnp.where(
                gap == 0, 2.0, 1.0
            )
            scores = (dot(qb, kb, ((1,), (1,))) * mixing).astype(BF)
            local_ref[n * tile : (n + 1) * tile, :] = dot(scores, v, ((1,), (0,)))


def middle_body(from_ref, state_ref, par_ref, message_ref, *, span, context_rows):
    nz, nx = from_ref.shape[0], message_ref.shape[0]
    rate_f, rate_b, zf, xf = (par_ref[k : k + 1, :] for k in range(4))

    def power(rate, blocks):
        kept = jnp.exp(-rate * (span * jnp.maximum(blocks, 0.0)))
        return jnp.where(blocks >= 0, kept, 0.0)

    sum_f = jnp.zeros((HEAD_DIM, HEAD_DIM), F32)
    sum_b = jnp.zeros((HEAD_DIM, HEAD_DIM), F32)
    for n in range(nz):
        s = from_ref[n, :HEAD_DIM, :].astype(F32)
        sum_f = sum_f + power(rate_f, nx * (zf - 1.0 - n)) * s
        sum_b = sum_b + power(rate_b, nx * (n - zf - 1.0)) * s
    total = float(context_rows * nz * nx)
    keys, values, at = [], [], []
    for n in range(nz):
        keys.append(from_ref[n, HEAD_DIM : HEAD_DIM + context_rows, :].astype(F32))
        values.append(from_ref[n, HEAD_DIM + context_rows :, :])
        at.append(
            lax.broadcasted_iota(jnp.int32, (context_rows, HEAD_DIM), 0).astype(F32)
            + context_rows * (nx * n + xf)
        )
    ck = jnp.concatenate(keys, 0) * (HEAD_DIM ** (-0.5) * CONTEXT_LIFT)
    cv = jnp.concatenate(values, 0)
    at = jnp.concatenate(at, 0)
    context_f = dot((ck * jnp.exp(-rate_f * (total - 1.0 - at))).astype(BF), cv, ((0,), (0,)))
    context_b = dot((ck * jnp.exp(-rate_b * at)).astype(BF), cv, ((0,), (0,)))
    own_f, own_b = state_ref[0], state_ref[1]
    for n in range(nx):
        message_ref[n, :HEAD_DIM, :] = (
            power(rate_f, nx - 1.0 + n - xf) * sum_f
            + power(rate_f, n - 1.0 - xf) * own_f
            + power(rate_f, nx * zf + n) * context_f
        ).astype(BF)
        message_ref[n, HEAD_DIM:, :] = (
            power(rate_b, nx - 1.0 + xf - n) * sum_b
            + power(rate_b, xf - n - 1.0) * own_b
            + power(rate_b, nx * nz - 1.0 - nx * zf - n) * context_b
        ).astype(BF)


def finish_body(from_ref, q_ref, g_ref, local_ref, par_ref, out_ref):
    tokens = q_ref.shape[0]
    rate_f, rate_b = par_ref[0:1, :], par_ref[1:2, :]
    incoming = from_ref[0].astype(F32)
    for n in range(1, from_ref.shape[0]):
        incoming = incoming + from_ref[n].astype(F32)
    row = lax.broadcasted_iota(jnp.int32, (tokens, HEAD_DIM), 0).astype(F32)
    q = q_ref[...]
    reads = jnp.concatenate(
        [
            (q * jnp.exp(-rate_f * (row + 1.0))).astype(BF),
            (q * jnp.exp(-rate_b * (tokens - row))).astype(BF),
        ],
        axis=1,
    )
    kept = local_ref[...] + dot(reads, incoming.astype(BF), ((1,), (0,)))
    kept = kept * lax.rsqrt(jnp.mean(kept * kept, axis=-1, keepdims=True) + EPS)
    g = g_ref[...].astype(F32)
    out_ref[...] = (g * (1.0 / (1.0 + jnp.exp(-g))) * kept).astype(BF)


def project_body(h_ref, w_ref, latent_ref, gate_ref, out_ref, h_scr):
    groups, _, width = h_ref.shape

    @pl.when(pl.program_id(0) == 0)
    def _():
        for k in range(groups):
            h_scr[:, k * width : (k + 1) * width] = h_ref[k]

    acc = dot(h_scr[...], w_ref[...], ((1,), (0,)))
    out_ref[...] = (latent_ref[...].astype(F32) + gate_ref[...] * acc).astype(BF)


def project(heads, weight, latent, gate):
    groups, rows, width = heads.shape
    depth, cols = weight.shape
    tile = 512
    return pl.pallas_call(
        project_body,
        grid=(cols // tile,),
        in_specs=[
            pl.BlockSpec((groups, rows, width), lambda j: (0, 0, 0)),
            pl.BlockSpec((depth, tile), lambda j: (0, j)),
            pl.BlockSpec((rows, tile), lambda j: (0, j)),
            pl.BlockSpec((1, tile), lambda j: (0, j)),
        ],
        out_specs=pl.BlockSpec((rows, tile), lambda j: (0, j)),
        out_shape=jax.ShapeDtypeStruct((rows, cols), BF),
        scratch_shapes=[pltpu.VMEM((rows, depth), BF)],
        name="project",
    )(heads, weight, latent, gate)


def whole(body, shapes, name, **options):
    return pl.pallas_call(body, out_shape=shapes, name=name, **options)


def local(
    latent,
    context,
    condition,
    context_condition,
    shift_weight,
    scale_weight,
    mod_gate_weight,
    norm_gain,
    query_weight,
    key_weight,
    value_weight,
    gate_weight,
    forward_decay,
    backward_decay,
    out_weight,
):
    z, x = lax.axis_index("z"), lax.axis_index("x")
    nz, nx, nt = lax.axis_size("z"), lax.axis_size("x"), lax.axis_size(TP)
    sp_index, sp_count = lax.axis_index(SP), nz * nx
    tokens, model = latent.shape
    context_rows = context.shape[0]
    mod_rows, mod_cols = shift_weight.shape

    full_weight = lax.all_gather(out_weight, TP, axis=0, tiled=True)

    conditions = jnp.stack([condition, context_condition])
    conditions = jnp.swapaxes(conditions.reshape(2, sp_count, mod_rows), 0, 1)
    memory = pltpu.MemorySpace
    partial = whole(
        partial_body,
        jax.ShapeDtypeStruct((sp_count, 8, mod_cols), F32),
        "partial",
        in_specs=[
            pl.BlockSpec(memory_space=memory.VMEM),
            pl.BlockSpec(memory_space=memory.SMEM),
        ]
        + [pl.BlockSpec(memory_space=memory.VMEM)] * 3,
    )(conditions, sp_index.reshape(1), shift_weight, scale_weight, mod_gate_weight)

    stacked = jnp.concatenate([query_weight, key_weight, value_weight, gate_weight], axis=1)
    cosine, sine = rope_tables(sp_index * tokens, tokens)
    numbers = jnp.stack(
        [forward_decay[0], backward_decay[0], z.astype(F32), x.astype(F32)]
        + [jnp.zeros((), F32)] * 4
    )
    par = jnp.broadcast_to(numbers[:, None], (8, HEAD_DIM))
    partial, stacked, cosine, sine, par, gain = lax.optimization_barrier(
        (partial, stacked, cosine, sine, par, norm_gain[None])
    )

    gathered = lax.all_to_all(partial, SP, split_axis=0, concat_axis=0, tiled=True)
    summed = whole(sum_body, jax.ShapeDtypeStruct((nt, 8, mod_cols), F32), "sum")(gathered)
    modulation = lax.all_to_all(summed, TP, split_axis=0, concat_axis=0, tiled=True)

    tile = 128
    pinned = lambda *shape: pl.BlockSpec(shape, lambda i: (0,) * len(shape))
    message_rows = HEAD_DIM + 2 * context_rows
    message, q, g, local_out, states, mod_gate = pl.pallas_call(
        front_body,
        grid=(tokens // tile,),
        in_specs=[
            pl.BlockSpec((tile, model), lambda i: (i, 0)),
            pinned(*context.shape),
            pinned(nt, 8, mod_cols),
            pinned(1, model),
            pinned(model, 4 * HEAD_DIM),
            pinned(tokens, HEAD_DIM),
            pinned(tokens, HEAD_DIM),
            pinned(8, HEAD_DIM),
        ],
        out_specs=[
            pinned(nz, message_rows, HEAD_DIM),
            pinned(tokens, HEAD_DIM),
            pinned(tokens, HEAD_DIM),
            pinned(tokens, HEAD_DIM),
            pinned(2, HEAD_DIM, HEAD_DIM),
            pinned(1, model),
        ],
        out_shape=[
            jax.ShapeDtypeStruct((nz, message_rows, HEAD_DIM), BF),
            jax.ShapeDtypeStruct((tokens, HEAD_DIM), F32),
            jax.ShapeDtypeStruct((tokens, HEAD_DIM), BF),
            jax.ShapeDtypeStruct((tokens, HEAD_DIM), F32),
            jax.ShapeDtypeStruct((2, HEAD_DIM, HEAD_DIM), F32),
            jax.ShapeDtypeStruct((1, model), F32),
        ],
        scratch_shapes=[
            pltpu.VMEM((tokens, HEAD_DIM), F32),
            pltpu.VMEM((tokens, HEAD_DIM), BF),
        ],
        name="front",
    )(latent, context, modulation, gain, stacked, cosine, sine, par)
    from_z = lax.all_to_all(message, "z", split_axis=0, concat_axis=0, tiled=True)
    message = whole(
        lambda *refs: middle_body(*refs, span=float(tokens), context_rows=context_rows),
        jax.ShapeDtypeStruct((nx, 2 * HEAD_DIM, HEAD_DIM), BF),
        "middle",
    )(from_z, states, par)
    from_x = lax.all_to_all(message, "x", split_axis=0, concat_axis=0, tiled=True)
    heads = whole(finish_body, jax.ShapeDtypeStruct((tokens, HEAD_DIM), BF), "finish")(
        from_x, q, g, local_out, par
    )
    heads, full_weight = lax.optimization_barrier((heads, full_weight))
    all_heads = lax.all_gather(heads, TP, axis=0, tiled=False)
    return project(all_heads, full_weight, latent, mod_gate)


def solution(mesh):
    torus = Mesh(mesh.devices.reshape(8, 4, 8, 2), ("z", "x", "y", "c"))
    rows, cols = P(SP, None), P(None, TP)
    both = P(SP, TP)
    in_specs = (
        (rows, rows, P(), P(), both, both, both, P(), cols, cols, cols, cols)
        + (P(TP), P(TP), P(TP, None))
    )
    return jax.shard_map(local, mesh=torus, in_specs=in_specs, out_specs=rows, check_vma=False)
```
